32 devices in a mesh: rep: 2 (over core), fs: 8 (over z, y), tp: 2 (over x).
Axes of the slice: x: 2, y: 2, z: 4, core: 2. Of those that a mesh axis runs over, the one named last changes fastest.
Arguments:
- tokens: bfloat16 [8192, 2048], P(('rep', 'fs')), may hold values from -6 to 6
- recurrence_branch_weight: bfloat16 [2048, 2048], P('fs', 'tp'), may hold values from -0.125 to 0.125
- gate_branch_weight: bfloat16 [2048, 2048], P('fs', 'tp'), may hold values from -0.125 to 0.125
- convolution_kernel: bfloat16 [4, 2048], P(None, 'tp'), may hold values from -3 to 3
- recurrence_gate_blockwise: bfloat16 [8, 256, 256], P('tp'), may hold values from -0.375 to 0.375
- input_gate_blockwise: bfloat16 [8, 256, 256], P('tp'), may hold values from -0.375 to 0.375
- channel_decay_param: float32 [2048], P('tp')
- token_decay_shift: float32 [8192, 2048], P(('rep', 'fs'), 'tp'), may hold values from -1 to 0
- recurrence_output_weight: bfloat16 [2048, 2048], P('tp', 'fs'), may hold values from -0.5 to 0.5
- first_norm_gain: float32 [2048], replicated, may hold values from 0.1 to 1.9
- feedforward_gate_weight: bfloat16 [2048, 5120], P('fs', 'tp'), may hold values from -0.125 to 0.125
- feedforward_up_weight: bfloat16 [2048, 5120], P('fs', 'tp'), may hold values from -0.125 to 0.125
- feedforward_down_weight: bfloat16 [5120, 2048], P('tp', 'fs'), may hold values from -0.15625 to 0.15625
- second_norm_gain: float32 [2048], replicated, may hold values from 0.1 to 1.9
Outputs:
- layer_out: bfloat16 [8192, 2048], P(('rep', 'fs', 'tp'))
The draws below stay inside these ranges and needn't reach their ends.
All inputs are finite; a program needn't handle non-finite values.
Results may differ from the reference program's by a relative error of at most 0.02.
Values may be sent and summed in bfloat16 or wider, within the bound.
A program may use at most 128 MiB of HBM per device.

```python
import math
import jax
import jax.numpy as jnp
from jax import lax

MODEL_WIDTH = 2048
FF = 5120
LRU_BLOCKS = 8
BLOCK = 256
CONV = 4
SEQUENCE_TOKENS = 512
RECURRENT_WIDTH = 2048
ROWS_ALL = 8192
N_TP = 2


def draw_channel_decay_param(key, part):
    key_flag = jax.random.fold_in(key, 11)
    key_slow = jax.random.fold_in(key, 12)
    key_fast = jax.random.fold_in(key, 13)
    quick = jax.random.randint(key_flag, (RECURRENT_WIDTH,), 0, 2) == 1
    slow_value = math.log(4.0 * SEQUENCE_TOKENS) + jax.random.uniform(key_slow, (RECURRENT_WIDTH,), jnp.float32, 0.0, 1.5)
    fast_value = math.log(4.0 * min(50.0, SEQUENCE_TOKENS / 4.0)) + jax.random.uniform(key_fast, (RECURRENT_WIDTH,), jnp.float32, -0.5, 0.5)
    return jnp.where(quick, fast_value, slow_value).astype(jnp.float32)


def draw_token_decay_shift(key, part):
    key_where = jax.random.fold_in(key, 21)
    key_depth = jax.random.fold_in(key, 22)
    struck = jax.random.randint(key_where, (ROWS_ALL, 1), 0, SEQUENCE_TOKENS) < 3
    depth = jax.random.uniform(key_depth, (ROWS_ALL, RECURRENT_WIDTH), jnp.float32, 0.22, 0.69)
    return jnp.where(struck, -depth, 0.0).astype(jnp.float32)


def block_levels(key, extent, cuts, low, top_value):
    level = 1.0
    for axis_at, parts in cuts:
        heights = jax.random.uniform(jax.random.fold_in(jax.random.fold_in(key, 6), axis_at), (parts,), jnp.float32, low / len(cuts), top_value / len(cuts))
        level = level * jnp.repeat(jnp.exp(heights), extent[axis_at] // parts).reshape((-1,) + (1,) * (len(extent) - 1 - axis_at))
    return level


def scatter_about(rng, shape, spread, bound, pieces=(), held_as=jnp.bfloat16):
    array = jax.random.normal(rng, shape, jnp.float32) * spread
    if len(pieces) > 0:
        array = block_levels(rng, shape, pieces, -0.22, 0.18) * array
    return jnp.clip(array, min=-bound, max=bound).astype(held_as)


def setup_inputs(seed: int = 0) -> dict:
    arg_keys = jax.random.split(jax.random.key(seed), 15)
    return {
        "tokens": scatter_about(arg_keys[0], (ROWS_ALL, MODEL_WIDTH), 1.0, 6.0, ((0, 16),)),
        "recurrence_branch_weight": scatter_about(arg_keys[1], (MODEL_WIDTH, RECURRENT_WIDTH), MODEL_WIDTH ** -0.5, 0.125, ((0, 8), (1, 2))),
        "gate_branch_weight": scatter_about(arg_keys[2], (MODEL_WIDTH, RECURRENT_WIDTH), MODEL_WIDTH ** -0.5, 0.125, ((0, 8), (1, 2))),
        "convolution_kernel": scatter_about(arg_keys[3], (CONV, RECURRENT_WIDTH), 0.5, 3.0, ((1, 2),)),
        "recurrence_gate_blockwise": scatter_about(arg_keys[4], (LRU_BLOCKS, BLOCK, BLOCK), BLOCK ** -0.5, 0.375, ((0, 2),)),
        "input_gate_blockwise": scatter_about(arg_keys[5], (LRU_BLOCKS, BLOCK, BLOCK), BLOCK ** -0.5, 0.375, ((0, 2),)),
        "channel_decay_param": draw_channel_decay_param(jax.random.fold_in(arg_keys[14], 71), 0),
        "token_decay_shift": draw_token_decay_shift(jax.random.fold_in(arg_keys[14], 71), 0),
        "recurrence_output_weight": scatter_about(arg_keys[8], (RECURRENT_WIDTH, MODEL_WIDTH), (RECURRENT_WIDTH // 16) ** -0.5, 0.5, ((0, 2), (1, 8))),
        "first_norm_gain": jnp.clip(1.0 + 0.18 * jax.random.normal(arg_keys[9], (MODEL_WIDTH,), jnp.float32), 0.1, 1.9),
        "feedforward_gate_weight": scatter_about(arg_keys[10], (MODEL_WIDTH, FF), MODEL_WIDTH ** -0.5, 0.125, ((0, 8), (1, 2))),
        "feedforward_up_weight": scatter_about(arg_keys[11], (MODEL_WIDTH, FF), MODEL_WIDTH ** -0.5, 0.125, ((0, 8), (1, 2))),
        "feedforward_down_weight": scatter_about(arg_keys[12], (FF, MODEL_WIDTH), (FF // 4) ** -0.5, 0.15625, ((0, 2), (1, 8))),
        "second_norm_gain": jnp.clip(1.0 + 0.18 * jax.random.normal(arg_keys[13], (MODEL_WIDTH,), jnp.float32), 0.1, 1.9),
    }


residual_scale = 1.4142135623730951

def layer_norm(values, gain):
    center = values - lax.optimization_barrier(jnp.mean(values, axis=-1, keepdims=True))
    variance = lax.optimization_barrier(jnp.mean(center * center, axis=-1, keepdims=True))
    return center * lax.rsqrt(variance + 1e-05) * gain

def grouped_product(left, right):
    width = left.shape[1] // N_TP
    total = jnp.zeros((left.shape[0], right.shape[1]), jnp.float32)
    for group in range(N_TP):
        term = jnp.dot(left[:, group * width:(group + 1) * width], right[group * width:(group + 1) * width], preferred_element_type=jnp.float32)
        term = lax.optimization_barrier(term.astype(jnp.bfloat16))
        total = total + term.astype(jnp.float32)
    return total

def combine(earlier, later):
    return (earlier[0] * later[0], later[0] * earlier[1] + later[1])

def single_sequence_layer(tokens, decay_added, recurrence_branch_weight, gate_branch_weight, convolution_kernel, recurrence_gate_blockwise, input_gate_blockwise, channel_decay_param, recurrence_output_weight, first_norm_gain, feedforward_gate_weight, feedforward_up_weight, feedforward_down_weight, second_norm_gain):
    length = tokens.shape[0]
    value_in = jnp.dot(tokens, recurrence_branch_weight, preferred_element_type=jnp.float32).astype(jnp.bfloat16)
    gate_in = jnp.dot(tokens, gate_branch_weight, preferred_element_type=jnp.float32).astype(jnp.bfloat16)
    padded = jnp.concatenate([jnp.zeros((CONV - 1, RECURRENT_WIDTH), jnp.float32), value_in.astype(jnp.float32)], axis=0)
    conv = jnp.zeros((length, RECURRENT_WIDTH), jnp.float32)
    for tap in range(CONV):
        conv = conv + padded[tap:tap + length] * convolution_kernel[tap].astype(jnp.float32)
    conv = conv.astype(jnp.bfloat16)
    blocked = conv.astype(jnp.float32).reshape(length, LRU_BLOCKS, BLOCK)
    recurrence_gate_value = jax.nn.sigmoid(jnp.einsum('rnk,nkj->rnj', blocked, recurrence_gate_blockwise.astype(jnp.float32)).reshape(length, RECURRENT_WIDTH))
    inlet = jax.nn.sigmoid(jnp.einsum('rnk,nkj->rnj', blocked, input_gate_blockwise.astype(jnp.float32)).reshape(length, RECURRENT_WIDTH))
    log_decay_factor = -8.0 * recurrence_gate_value * jax.nn.softplus(-channel_decay_param) + decay_added
    decay = jnp.exp(log_decay_factor)
    drive = jnp.sqrt(-jnp.expm1(2.0 * log_decay_factor)) * inlet * conv.astype(jnp.float32)
    _, state = lax.associative_scan(combine, (decay, drive), axis=0)
    branch = (state * jax.nn.gelu(gate_in.astype(jnp.float32))).astype(jnp.bfloat16)
    mix = grouped_product(branch, recurrence_output_weight)
    normed = layer_norm(residual_scale * tokens.astype(jnp.float32) + mix, first_norm_gain).astype(jnp.bfloat16)
    gate = jnp.dot(normed, feedforward_gate_weight, preferred_element_type=jnp.float32)
    upward = jnp.dot(normed, feedforward_up_weight, preferred_element_type=jnp.float32)
    hidden = (jax.nn.silu(gate) * upward).astype(jnp.bfloat16)
    ffn = grouped_product(hidden, feedforward_down_weight)
    return layer_norm(residual_scale * normed.astype(jnp.float32) + ffn, second_norm_gain).astype(jnp.bfloat16)

def reference(tokens, recurrence_branch_weight, gate_branch_weight, convolution_kernel, recurrence_gate_blockwise, input_gate_blockwise, channel_decay_param, token_decay_shift, recurrence_output_weight, first_norm_gain, feedforward_gate_weight, feedforward_up_weight, feedforward_down_weight, second_norm_gain):
    token_count = tokens.shape[0] // SEQUENCE_TOKENS

    def apply_layer(pair):
        return single_sequence_layer(pair[0], pair[1], recurrence_branch_weight, gate_branch_weight, convolution_kernel, recurrence_gate_blockwise, input_gate_blockwise, channel_decay_param, recurrence_output_weight, first_norm_gain, feedforward_gate_weight, feedforward_up_weight, feedforward_down_weight, second_norm_gain)
    layer_result = lax.map(apply_layer, (tokens.reshape(token_count, SEQUENCE_TOKENS, MODEL_WIDTH), token_decay_shift.reshape(token_count, SEQUENCE_TOKENS, RECURRENT_WIDTH)))
    return layer_result.reshape(token_count * SEQUENCE_TOKENS, MODEL_WIDTH)
```

```python
import functools

import jax
import jax.numpy as jnp
from jax import lax
from jax.experimental import pallas as pl
from jax.experimental.pallas import tpu as pltpu
from jax.sharding import PartitionSpec as P

residual_scale = 1.4142135623730951


VMEM_BYTES = 60 * 1024 * 1024


def layer_norm(values, gain):
    center = values - jnp.mean(values, axis=-1, keepdims=True)
    variance = jnp.mean(center * center, axis=-1, keepdims=True)
    return center * lax.rsqrt(variance + 1e-05) * gain


def direct_plan():
    count = lax.axis_size("fs")
    return lax.axis_size("rep") == 2 and count % 2 == 0 and count <= 8


def gather_parts(shard):
    count = lax.axis_size("fs")
    outer = count // 2
    mine = [shard]
    for step in range(1, outer):
        pairs = [
            (at * 2 + side, ((at - step) % outer) * 2 + side)
            for at in range(outer)
            for side in range(2)
        ]
        mine.append(lax.ppermute(shard, "fs", pairs))
    swap = [(at, at ^ 1) for at in range(count)]
    mine = mine + [lax.ppermute(part, "fs", swap) for part in mine]
    other = [lax.ppermute(part, "rep", [(0, 1), (1, 0)]) for part in mine]
    return mine, other


def part_owners():
    count = lax.axis_size("fs")
    outer = count // 2
    me = lax.axis_index("fs")
    at, side = me // 2, me % 2
    return [
        ((at + step) % outer) * 2 + (side if flip == 0 else 1 - side)
        for flip in range(2)
        for step in range(outer)
    ]


def gather_two(first, second, axis):
    if direct_plan():
        core = lax.axis_index("rep")
        mine, other = gather_parts(jnp.where(core == 0, first, second))
        return mine, other, part_owners(), core
    return (
        [lax.all_gather(first, "fs", axis=axis, tiled=True)],
        [lax.all_gather(second, "fs", axis=axis, tiled=True)],
        [jnp.int32(0)],
        jnp.int32(0),
    )


def gather_halves(weight):
    half = weight.shape[0] // 2
    return gather_two(weight[:half], weight[half:], 1)


def scalars(owners, swapped):
    return jnp.stack([jnp.asarray(v, jnp.int32) for v in [swapped, *owners]])


def split_product(meta, left_ref, part_refs):
    total = None
    for at, part in enumerate(part_refs):
        depth = part.shape[0]
        columns = pl.ds(pl.multiple_of(meta[1 + at] * depth, depth), depth)
        term = jnp.dot(left_ref[:, columns], part[...], preferred_element_type=jnp.float32)
        total = term if total is None else total + term
    return total


def shifted(values, step, fill):
    rows = lax.broadcasted_iota(jnp.int32, values.shape, 0)
    return jnp.where(rows < step, fill, pltpu.roll(values, step, 0))


def sigmoid(values):
    return 1.0 / (1.0 + jnp.exp(-values))


def recurrence_kernel(count, meta, x_ref, taps_ref, rate_ref, inlet_ref, plus_ref, shift_ref, *refs):
    mine, other, out_ref = refs[:count], refs[count : 2 * count], refs[-1]
    first = split_product(meta, x_ref, mine)
    second = split_product(meta, x_ref, other)
    swapped = meta[0] == 1
    value_in = jnp.where(swapped, second, first).astype(jnp.bfloat16).astype(jnp.float32)
    gate_in = jnp.where(swapped, first, second).astype(jnp.bfloat16).astype(jnp.float32)
    taps = taps_ref[...].astype(jnp.float32)
    depth = taps.shape[0]
    conv = None
    for tap in range(depth):
        lag = depth - 1 - tap
        moved = value_in if lag == 0 else shifted(value_in, lag, 0.0)
        term = moved * taps[tap : tap + 1, :]
        conv = term if conv is None else conv + term
    conv = conv.astype(jnp.bfloat16)
    rate = sigmoid(jnp.dot(conv, rate_ref[0], preferred_element_type=jnp.float32))
    inlet = sigmoid(jnp.dot(conv, inlet_ref[0], preferred_element_type=jnp.float32))
    log_decay = -8.0 * rate * plus_ref[...] + shift_ref[...]
    decay = jnp.exp(log_decay)
    twice = 2.0 * log_decay
    series = jnp.ones_like(twice)
    for order in range(8, 1, -1):
        series = 1.0 + twice * series * (1.0 / order)
    lost = jnp.where(twice > -0.3, -twice * series, 1.0 - jnp.exp(twice))
    state = jnp.sqrt(lost) * inlet * conv.astype(jnp.float32)
    step = 1
    while step < state.shape[0]:
        state = state + decay * shifted(state, step, 0.0)
        if 2 * step < state.shape[0]:
            decay = decay * shifted(decay, step, 1.0)
        step *= 2
    gelu = 0.5 * gate_in * (
        1.0 + jnp.tanh(0.7978845608028654 * (gate_in + 0.044715 * gate_in * gate_in * gate_in))
    )
    out_ref[...] = (state * gelu).astype(jnp.bfloat16)


def recurrence(tokens, mine, other, meta, taps, rate_blocks, inlet_blocks, plus, shift):
    length, width = tokens.shape
    block = rate_blocks.shape[1]
    blocks = rate_blocks.shape[0]
    parts = [pl.BlockSpec((p.shape[0], block), lambda i: (0, i)) for p in [*mine, *other]]
    column = lambda rows: pl.BlockSpec((rows, block), lambda i: (0, i))
    square = pl.BlockSpec((1, block, block), lambda i: (i, 0, 0))
    return pl.pallas_call(
        functools.partial(recurrence_kernel, len(mine)),
        grid=(blocks,),
        in_specs=[
            pl.BlockSpec(memory_space=pltpu.SMEM),
            pl.BlockSpec((length, width), lambda i: (0, 0)),
            column(taps.shape[0]),
            square,
            square,
            column(1),
            column(length),
            *parts,
        ],
        out_specs=column(length),
        out_shape=jax.ShapeDtypeStruct((length, block * blocks), jnp.bfloat16),
        cost_estimate=pl.CostEstimate(
            flops=4 * length * width * block * blocks,
            bytes_accessed=4 * width * block * blocks + 8 * length * block * blocks,
            transcendentals=0,
        ),
        compiler_params=pltpu.CompilerParams(vmem_limit_bytes=VMEM_BYTES),
    )(meta, tokens, taps, rate_blocks, inlet_blocks, plus, shift, *mine, *other)


def hidden_kernel(count, meta, x_ref, *refs):
    mine, other, out_ref = refs[:count], refs[count : 2 * count], refs[-1]
    first = split_product(meta, x_ref, mine)
    second = split_product(meta, x_ref, other)
    swapped = meta[0] == 1
    gate = jnp.where(swapped, second, first)
    upward = jnp.where(swapped, first, second)
    out_ref[...] = (gate * sigmoid(gate) * upward).astype(jnp.bfloat16)


def hidden_units(normed, mine, other, meta):
    length, width = normed.shape
    units = mine[0].shape[1]
    tile = next(t for t in (512, 640, 256, 128, units) if units % t == 0)
    return pl.pallas_call(
        functools.partial(hidden_kernel, len(mine)),
        grid=(units // tile,),
        in_specs=[
            pl.BlockSpec(memory_space=pltpu.SMEM),
            pl.BlockSpec((length, width), lambda i: (0, 0)),
            *[pl.BlockSpec((p.shape[0], tile), lambda i: (0, i)) for p in [*mine, *other]],
        ],
        out_specs=pl.BlockSpec((length, tile), lambda i: (0, i)),
        out_shape=jax.ShapeDtypeStruct((length, units), jnp.bfloat16),
        cost_estimate=pl.CostEstimate(
            flops=4 * length * width * units, bytes_accessed=4 * width * units, transcendentals=0
        ),
        compiler_params=pltpu.CompilerParams(vmem_limit_bytes=VMEM_BYTES),
    )(meta, normed, *mine, *other)


def outward_kernel(count, meta, left_ref, *refs):
    mine, other, out_ref = refs[:count], refs[count : 2 * count], refs[-1]
    half = mine[0].shape[0]
    near = pl.ds(pl.multiple_of(meta[0] * half, 128), half)
    far = pl.ds(pl.multiple_of((1 - meta[0]) * half, 128), half)
    for at in range(count):
        total = jnp.dot(left_ref[:, near], mine[at][...], preferred_element_type=jnp.float32)
        total += jnp.dot(left_ref[:, far], other[at][...], preferred_element_type=jnp.float32)
        columns = mine[at].shape[1]
        start = pl.multiple_of(meta[1 + at] * columns, 128)
        out_ref[:, pl.ds(start, columns)] = total.astype(jnp.bfloat16)


def outward(left, mine, other, meta):
    length, depth = left.shape
    width = sum(p.shape[1] for p in mine)
    rows = min(length, 256)
    whole = [pl.BlockSpec(p.shape, lambda i: (0, 0)) for p in [*mine, *other]]
    return pl.pallas_call(
        functools.partial(outward_kernel, len(mine)),
        grid=(length // rows,),
        in_specs=[
            pl.BlockSpec(memory_space=pltpu.SMEM),
            pl.BlockSpec((rows, depth), lambda i: (i, 0)),
            *whole,
        ],
        out_specs=pl.BlockSpec((rows, width), lambda i: (i, 0)),
        out_shape=jax.ShapeDtypeStruct((length, width), jnp.bfloat16),
        cost_estimate=pl.CostEstimate(
            flops=2 * length * width * depth, bytes_accessed=2 * width * depth, transcendentals=0
        ),
        compiler_params=pltpu.CompilerParams(vmem_limit_bytes=VMEM_BYTES),
    )(meta, left, *mine, *other)


def add_groups(terms):
    groups = lax.axis_size("tp")
    if groups != 2:
        return lax.psum_scatter(terms, "tp", scatter_dimension=0, tiled=True).astype(jnp.float32)
    share = terms.shape[0] // 2
    me = lax.axis_index("tp")
    away = lax.dynamic_slice_in_dim(terms, (1 - me) * share, share, 0)
    own = lax.dynamic_slice_in_dim(terms, me * share, share, 0)
    came = lax.ppermute(away, "tp", [(0, 1), (1, 0)])
    return own.astype(jnp.float32) + came.astype(jnp.float32)


def all_rows(rows):
    if lax.axis_size("tp") != 2:
        return lax.all_gather(rows, "tp", axis=0, tiled=True)
    came = lax.ppermute(rows, "tp", [(0, 1), (1, 0)])
    low = lax.axis_index("tp") == 0
    return jnp.concatenate([jnp.where(low, rows, came), jnp.where(low, came, rows)], axis=0)


def local(
    tokens,
    recurrence_branch_weight,
    gate_branch_weight,
    convolution_kernel,
    recurrence_gate_blockwise,
    input_gate_blockwise,
    channel_decay_param,
    token_decay_shift,
    recurrence_output_weight,
    first_norm_gain,
    feedforward_gate_weight,
    feedforward_up_weight,
    feedforward_down_weight,
    second_norm_gain,
):
    share = tokens.shape[0] // lax.axis_size("tp")
    offset = lax.axis_index("tp") * share
    in_mine, in_other, owners, swapped = gather_two(recurrence_branch_weight, gate_branch_weight, 0)
    out_mine, out_other, _, _ = gather_halves(recurrence_output_weight)
    ff_mine, ff_other, _, _ = gather_two(feedforward_gate_weight, feedforward_up_weight, 0)
    down_mine, down_other, _, _ = gather_halves(feedforward_down_weight)
    meta = scalars(owners, swapped)
    branch = recurrence(
        tokens,
        in_mine,
        in_other,
        meta,
        convolution_kernel,
        recurrence_gate_blockwise,
        input_gate_blockwise,
        jax.nn.softplus(-channel_decay_param)[None, :],
        token_decay_shift,
    )
    mix = add_groups(outward(branch, out_mine, out_other, meta))
    own_tokens = lax.dynamic_slice_in_dim(tokens, offset, share, 0)
    normed = layer_norm(
        residual_scale * own_tokens.astype(jnp.float32) + mix, first_norm_gain
    ).astype(jnp.bfloat16)
    hidden = hidden_units(all_rows(normed), ff_mine, ff_other, meta)
    ffn = add_groups(outward(hidden, down_mine, down_other, meta))
    return layer_norm(residual_scale * normed.astype(jnp.float32) + ffn, second_norm_gain).astype(
        jnp.bfloat16
    )


def solution(mesh):
    return jax.shard_map(
        local,
        mesh=mesh,
        in_specs=(
            P(("rep", "fs"), None),
            P("fs", "tp"),
            P("fs", "tp"),
            P(None, "tp"),
            P("tp", None, None),
            P("tp", None, None),
            P("tp"),
            P(("rep", "fs"), "tp"),
            P("tp", "fs"),
            P(),
            P("fs", "tp"),
            P("fs", "tp"),
            P("tp", "fs"),
            P(),
        ),
        out_specs=P(("rep", "fs", "tp"), None),
        check_vma=False,
    )
```

```python
import functools

import jax
import jax.numpy as jnp
from jax import lax
from jax.experimental import pallas as pl
from jax.experimental.pallas import tpu as pltpu
from jax.sharding import PartitionSpec as P


residual_scale = 1.4142135623730951


VMEM_BYTES = 60 * 1024 * 1024


def layer_norm(values, gain):
    center = values - jnp.mean(values, axis=-1, keepdims=True)
    variance = jnp.mean(center * center, axis=-1, keepdims=True)
    return center * lax.rsqrt(variance + 1e-05) * gain


def direct_plan():
    count = lax.axis_size("fs")
    return lax.axis_size("rep") == 2 and count % 2 == 0 and count <= 8


def visit_order(outer):
    return sorted(range(1, outer), key=lambda step: min(step, outer - step))


def gather_parts(shard):
    count = lax.axis_size("fs")
    outer = count // 2
    swap = [(at, at ^ 1) for at in range(count)]
    near = {0: shard}
    for step in visit_order(outer):
        pairs = [
            (at * 2 + side, ((at - step) % outer) * 2 + side)
            for at in range(outer)
            for side in range(2)
        ]
        near[step] = lax.ppermute(shard, "fs", pairs)
    far = {}
    for step in range(outer):
        far[step] = lax.ppermute(near[step], "fs", swap)
    mine = [near[step] for step in range(outer)] + [far[step] for step in range(outer)]
    other = []
    for part in mine:
        other.append(lax.ppermute(part, "rep", [(0, 1), (1, 0)]))
    return mine, other


def part_owners():
    count = lax.axis_size("fs")
    outer = count // 2
    me = lax.axis_index("fs")
    at, side = me // 2, me % 2
    return [
        ((at + step) % outer) * 2 + (side if flip == 0 else 1 - side)
        for flip in range(2)
        for step in range(outer)
    ]


def gather_two(first, second, axis):
    if direct_plan():
        core = lax.axis_index("rep")
        mine, other = gather_parts(jnp.where(core == 0, first, second))
        return mine, other, part_owners(), core
    return (
        [lax.all_gather(first, "fs", axis=axis, tiled=True)],
        [lax.all_gather(second, "fs", axis=axis, tiled=True)],
        [jnp.int32(0)],
        jnp.int32(0),
    )


def gather_halves(weight):
    half = weight.shape[0] // 2
    return gather_two(weight[:half], weight[half:], 1)


def scalars(owners, swapped):
    return jnp.stack([jnp.asarray(v, jnp.int32) for v in [swapped, *owners]])


def split_product(meta, left_ref, part_refs):
    total = None
    for at, part in enumerate(part_refs):
        depth = part.shape[0]
        columns = pl.ds(pl.multiple_of(meta[1 + at] * depth, depth), depth)
        term = jnp.dot(left_ref[:, columns], part[...], preferred_element_type=jnp.float32)
        total = term if total is None else total + term
    return total


def shifted(values, step, fill):
    rows = lax.broadcasted_iota(jnp.int32, values.shape, 0)
    return jnp.where(rows < step, fill, pltpu.roll(values, step, 0))


def sigmoid(values):
    return 1.0 / (1.0 + jnp.exp(-values))


def recurrence_kernel(count, meta, x_ref, taps_ref, rate_ref, inlet_ref, plus_ref, shift_ref, *refs):
    mine, other, out_ref = refs[:count], refs[count : 2 * count], refs[-1]
    first = split_product(meta, x_ref, mine)
    second = split_product(meta, x_ref, other)
    swapped = meta[0] == 1
    value_in = jnp.where(swapped, second, first).astype(jnp.bfloat16).astype(jnp.float32)
    gate_in = jnp.where(swapped, first, second).astype(jnp.bfloat16).astype(jnp.float32)
    taps = taps_ref[...].astype(jnp.float32)
    depth = taps.shape[0]
    conv = None
    for tap in range(depth):
        lag = depth - 1 - tap
        moved = value_in if lag == 0 else shifted(value_in, lag, 0.0)
        term = moved * taps[tap : tap + 1, :]
        conv = term if conv is None else conv + term
    conv = conv.astype(jnp.bfloat16)
    rate = sigmoid(jnp.dot(conv, rate_ref[0], preferred_element_type=jnp.float32))
    inlet = sigmoid(jnp.dot(conv, inlet_ref[0], preferred_element_type=jnp.float32))
    log_decay = -8.0 * rate * plus_ref[...] + shift_ref[...]
    decay = jnp.exp(log_decay)
    twice = 2.0 * log_decay
    series = jnp.ones_like(twice)
    for order in range(8, 1, -1):
        series = 1.0 + twice * series * (1.0 / order)
    lost = jnp.where(twice > -0.3, -twice * series, 1.0 - jnp.exp(twice))
    state = jnp.sqrt(lost) * inlet * conv.astype(jnp.float32)
    step = 1
    while step < state.shape[0]:
        state = state + decay * shifted(state, step, 0.0)
        if 2 * step < state.shape[0]:
            decay = decay * shifted(decay, step, 1.0)
        step *= 2
    gelu = 0.5 * gate_in * (
        1.0 + jnp.tanh(0.7978845608028654 * (gate_in + 0.044715 * gate_in * gate_in * gate_in))
    )
    out_ref[...] = (state * gelu).astype(jnp.bfloat16)


def recurrence(tokens, mine, other, meta, taps, rate_blocks, inlet_blocks, plus, shift):
    length, width = tokens.shape
    block = rate_blocks.shape[1]
    blocks = rate_blocks.shape[0]
    parts = [pl.BlockSpec((p.shape[0], block), lambda i: (0, i)) for p in [*mine, *other]]
    column = lambda rows: pl.BlockSpec((rows, block), lambda i: (0, i))
    square = pl.BlockSpec((1, block, block), lambda i: (i, 0, 0))
    return pl.pallas_call(
        functools.partial(recurrence_kernel, len(mine)),
        grid=(blocks,),
        in_specs=[
            pl.BlockSpec(memory_space=pltpu.SMEM),
            pl.BlockSpec((length, width), lambda i: (0, 0)),
            column(taps.shape[0]),
            square,
            square,
            column(1),
            column(length),
            *parts,
        ],
        out_specs=column(length),
        out_shape=jax.ShapeDtypeStruct((length, block * blocks), jnp.bfloat16),
        cost_estimate=pl.CostEstimate(
            flops=4 * length * width * block * blocks,
            bytes_accessed=4 * width * block * blocks + 8 * length * block * blocks,
            transcendentals=0,
        ),
        compiler_params=pltpu.CompilerParams(vmem_limit_bytes=VMEM_BYTES),
    )(meta, tokens, taps, rate_blocks, inlet_blocks, plus, shift, *mine, *other)


def hidden_kernel(count, meta, x_ref, *refs):
    mine, other, out_ref = refs[:count], refs[count : 2 * count], refs[-1]
    first = split_product(meta, x_ref, mine)
    second = split_product(meta, x_ref, other)
    swapped = meta[0] == 1
    gate = jnp.where(swapped, second, first)
    upward = jnp.where(swapped, first, second)
    out_ref[...] = (gate * sigmoid(gate) * upward).astype(jnp.bfloat16)


def hidden_units(normed, mine, other, meta):
    length, width = normed.shape
    units = mine[0].shape[1]
    tile = next(t for t in (512, 640, 256, 128, units) if units % t == 0)
    return pl.pallas_call(
        functools.partial(hidden_kernel, len(mine)),
        grid=(units // tile,),
        in_specs=[
            pl.BlockSpec(memory_space=pltpu.SMEM),
            pl.BlockSpec((length, width), lambda i: (0, 0)),
            *[pl.BlockSpec((p.shape[0], tile), lambda i: (0, i)) for p in [*mine, *other]],
        ],
        out_specs=pl.BlockSpec((length, tile), lambda i: (0, i)),
        out_shape=jax.ShapeDtypeStruct((length, units), jnp.bfloat16),
        cost_estimate=pl.CostEstimate(
            flops=4 * length * width * units, bytes_accessed=4 * width * units, transcendentals=0
        ),
        compiler_params=pltpu.CompilerParams(vmem_limit_bytes=VMEM_BYTES),
    )(meta, normed, *mine, *other)


def outward_kernel(count, meta, left_ref, *refs):
    mine, other, out_ref = refs[:count], refs[count : 2 * count], refs[-1]
    half = mine[0].shape[0]
    near = pl.ds(pl.multiple_of(meta[0] * half, 128), half)
    far = pl.ds(pl.multiple_of((1 - meta[0]) * half, 128), half)
    start = 0
    for at in range(count):
        total = jnp.dot(left_ref[:, near], mine[at][...], preferred_element_type=jnp.float32)
        total += jnp.dot(left_ref[:, far], other[at][...], preferred_element_type=jnp.float32)
        columns = mine[at].shape[1]
        out_ref[:, start : start + columns] = total.astype(jnp.bfloat16)
        start += columns


def outward(left, mine, other, meta):
    length, depth = left.shape
    width = sum(p.shape[1] for p in mine)
    rows = min(length, 256)
    whole = [pl.BlockSpec(p.shape, lambda i: (0, 0)) for p in [*mine, *other]]
    return pl.pallas_call(
        functools.partial(outward_kernel, len(mine)),
        grid=(length // rows,),
        in_specs=[
            pl.BlockSpec(memory_space=pltpu.SMEM),
            pl.BlockSpec((rows, depth), lambda i: (i, 0)),
            *whole,
        ],
        out_specs=pl.BlockSpec((rows, width), lambda i: (i, 0)),
        out_shape=jax.ShapeDtypeStruct((length, width), jnp.bfloat16),
        cost_estimate=pl.CostEstimate(
            flops=2 * length * width * depth, bytes_accessed=2 * width * depth, transcendentals=0
        ),
        compiler_params=pltpu.CompilerParams(vmem_limit_bytes=VMEM_BYTES),
    )(meta, left, *mine, *other)


def add_groups(terms):
    groups = lax.axis_size("tp")
    if groups != 2:
        return lax.psum_scatter(terms, "tp", scatter_dimension=0, tiled=True).astype(jnp.float32)
    share = terms.shape[0] // 2
    me = lax.axis_index("tp")
    away = lax.dynamic_slice_in_dim(terms, (1 - me) * share, share, 0)
    own = lax.dynamic_slice_in_dim(terms, me * share, share, 0)
    came = lax.ppermute(away, "tp", [(0, 1), (1, 0)])
    return own.astype(jnp.float32) + came.astype(jnp.float32)


def grouped_outward(left, mine, other, owners, meta, cut):
    count = len(mine)
    if count == 1:
        return add_groups(outward(left, mine, other, meta))
    outer = count // 2
    chunks = [list(range(count))]
    if cut:
        steps = visit_order(outer)
        last, late = steps[-1], [outer + step for step in steps]
        early = [at for at in range(outer + 1) if at != last]
        chunks = [chunk for chunk in (early, late[:-1], [last], late[-1:]) if chunk]
    width = mine[0].shape[1]
    total = jnp.zeros((left.shape[0] // lax.axis_size("tp"), width * count), jnp.float32)
    for chunk in chunks:
        terms = outward(left, [mine[at] for at in chunk], [other[at] for at in chunk], meta)
        block = add_groups(terms)
        for place, at in enumerate(chunk):
            piece = block[:, place * width : (place + 1) * width]
            total = lax.dynamic_update_slice_in_dim(total, piece, owners[at] * width, 1)
    return total


def all_rows(rows):
    if lax.axis_size("tp") != 2:
        return lax.all_gather(rows, "tp", axis=0, tiled=True)
    came = lax.ppermute(rows, "tp", [(0, 1), (1, 0)])
    low = lax.axis_index("tp") == 0
    return jnp.concatenate([jnp.where(low, rows, came), jnp.where(low, came, rows)], axis=0)


def layer(
    tokens,
    recurrence_branch_weight,
    gate_branch_weight,
    convolution_kernel,
    recurrence_gate_blockwise,
    input_gate_blockwise,
    channel_decay_param,
    token_decay_shift,
    recurrence_output_weight,
    first_norm_gain,
    feedforward_gate_weight,
    feedforward_up_weight,
    feedforward_down_weight,
    second_norm_gain,
):
    share = tokens.shape[0] // lax.axis_size("tp")
    offset = lax.axis_index("tp") * share
    in_mine, in_other, owners, swapped = gather_two(recurrence_branch_weight, gate_branch_weight, 0)
    out_mine, out_other, _, _ = gather_halves(recurrence_output_weight)
    ff_mine, ff_other, _, _ = gather_two(feedforward_gate_weight, feedforward_up_weight, 0)
    down_mine, down_other, _, _ = gather_halves(feedforward_down_weight)
    meta = scalars(owners, swapped)
    branch = recurrence(
        tokens,
        in_mine,
        in_other,
        meta,
        convolution_kernel,
        recurrence_gate_blockwise,
        input_gate_blockwise,
        jax.nn.softplus(-channel_decay_param)[None, :],
        token_decay_shift,
    )
    mix = grouped_outward(branch, out_mine, out_other, owners, meta, False)
    own_tokens = lax.dynamic_slice_in_dim(tokens, offset, share, 0)
    normed = layer_norm(
        residual_scale * own_tokens.astype(jnp.float32) + mix, first_norm_gain
    ).astype(jnp.bfloat16)
    rows = all_rows(normed)
    hidden = hidden_units(rows, ff_mine, ff_other, meta)
    ffn = grouped_outward(hidden, down_mine, down_other, owners, meta, True)
    return layer_norm(residual_scale * normed.astype(jnp.float32) + ffn, second_norm_gain).astype(
        jnp.bfloat16
    )


def solution(mesh):
    return jax.shard_map(
        layer,
        mesh=mesh,
        in_specs=(
            P(("rep", "fs"), None),
            P("fs", "tp"),
            P("fs", "tp"),
            P(None, "tp"),
            P("tp", None, None),
            P("tp", None, None),
            P("tp"),
            P(("rep", "fs"), "tp"),
            P("tp", "fs"),
            P(),
            P("fs", "tp"),
            P("fs", "tp"),
            P("tp", "fs"),
            P(),
        ),
        out_specs=P(("rep", "fs", "tp"), None),
        check_vma=False,
    )
```

```python
import functools

import jax
import jax.numpy as jnp
from jax import lax
from jax.experimental import pallas as pl
from jax.experimental.pallas import tpu as pltpu
from jax.sharding import PartitionSpec as P


residual_scale = 1.4142135623730951


VMEM_BYTES = 60 * 1024 * 1024


def layer_norm(values, gain):
    center = values - jnp.mean(values, axis=-1, keepdims=True)
    variance = jnp.mean(center * center, axis=-1, keepdims=True)
    return center * lax.rsqrt(variance + 1e-05) * gain


def direct_plan():
    count = lax.axis_size("fs")
    return lax.axis_size("rep") == 2 and count % 2 == 0 and count <= 8


def visit_order(outer):
    return sorted(range(1, outer), key=lambda step: min(step, outer - step))


def gather_parts(shard):
    count = lax.axis_size("fs")
    outer = count // 2
    swap = [(at, at ^ 1) for at in range(count)]
    near = {0: shard}
    for step in visit_order(outer):
        held, hop = (shard, step) if min(step, outer - step) == 1 else (near[step - 1], 1)
        pairs = [
            (at * 2 + side, ((at - hop) % outer) * 2 + side)
            for at in range(outer)
            for side in range(2)
        ]
        near[step] = lax.ppermute(held, "fs", pairs)
    far = {}
    for step in range(outer):
        far[step] = lax.ppermute(near[step], "fs", swap)
    mine = [near[step] for step in range(outer)] + [far[step] for step in range(outer)]
    other = []
    for part in mine:
        other.append(lax.ppermute(part, "rep", [(0, 1), (1, 0)]))
    return mine, other


def part_owners():
    count = lax.axis_size("fs")
    outer = count // 2
    me = lax.axis_index("fs")
    at, side = me // 2, me % 2
    return [
        ((at + step) % outer) * 2 + (side if flip == 0 else 1 - side)
        for flip in range(2)
        for step in range(outer)
    ]


def gather_two(first, second, axis):
    if direct_plan():
        core = lax.axis_index("rep")
        mine, other = gather_parts(jnp.where(core == 0, first, second))
        return mine, other, part_owners(), core
    return (
        [lax.all_gather(first, "fs", axis=axis, tiled=True)],
        [lax.all_gather(second, "fs", axis=axis, tiled=True)],
        [jnp.int32(0)],
        jnp.int32(0),
    )


def gather_halves(weight):
    half = weight.shape[0] // 2
    return gather_two(weight[:half], weight[half:], 1)


def scalars(owners, swapped):
    return jnp.stack([jnp.asarray(v, jnp.int32) for v in [swapped, *owners]])


def split_product(meta, left_ref, part_refs):
    total = None
    for at, part in enumerate(part_refs):
        depth = part.shape[0]
        columns = pl.ds(pl.multiple_of(meta[1 + at] * depth, depth), depth)
        term = jnp.dot(left_ref[:, columns], part[...], preferred_element_type=jnp.float32)
        total = term if total is None else total + term
    return total


def shifted(values, step, fill):
    rows = lax.broadcasted_iota(jnp.int32, values.shape, 0)
    return jnp.where(rows < step, fill, pltpu.roll(values, step, 0))


def sigmoid(values):
    return 1.0 / (1.0 + jnp.exp(-values))


def recurrence_kernel(count, meta, x_ref, taps_ref, rate_ref, inlet_ref, plus_ref, shift_ref, *refs):
    mine, other, out_ref = refs[:count], refs[count : 2 * count], refs[-1]
    first = split_product(meta, x_ref, mine)
    second = split_product(meta, x_ref, other)
    swapped = meta[0] == 1
    value_in = jnp.where(swapped, second, first).astype(jnp.bfloat16).astype(jnp.float32)
    gate_in = jnp.where(swapped, first, second).astype(jnp.bfloat16).astype(jnp.float32)
    taps = taps_ref[...].astype(jnp.float32)
    depth = taps.shape[0]
    conv = None
    for tap in range(depth):
        lag = depth - 1 - tap
        moved = value_in if lag == 0 else shifted(value_in, lag, 0.0)
        term = moved * taps[tap : tap + 1, :]
        conv = term if conv is None else conv + term
    conv = conv.astype(jnp.bfloat16)
    rate = sigmoid(jnp.dot(conv, rate_ref[0], preferred_element_type=jnp.float32))
    inlet = sigmoid(jnp.dot(conv, inlet_ref[0], preferred_element_type=jnp.float32))
    log_decay = -8.0 * rate * plus_ref[...] + shift_ref[...]
    decay = jnp.exp(log_decay)
    twice = 2.0 * log_decay
    series = jnp.ones_like(twice)
    for order in range(8, 1, -1):
        series = 1.0 + twice * series * (1.0 / order)
    lost = jnp.where(twice > -0.3, -twice * series, 1.0 - jnp.exp(twice))
    state = jnp.sqrt(lost) * inlet * conv.astype(jnp.float32)
    step = 1
    while step < state.shape[0]:
        state = state + decay * shifted(state, step, 0.0)
        if 2 * step < state.shape[0]:
            decay = decay * shifted(decay, step, 1.0)
        step *= 2
    gelu = 0.5 * gate_in * (
        1.0 + jnp.tanh(0.7978845608028654 * (gate_in + 0.044715 * gate_in * gate_in * gate_in))
    )
    out_ref[...] = (state * gelu).astype(jnp.bfloat16)


def recurrence(tokens, mine, other, meta, taps, rate_blocks, inlet_blocks, plus, shift):
    length, width = tokens.shape
    block = rate_blocks.shape[1]
    blocks = rate_blocks.shape[0]
    parts = [pl.BlockSpec((p.shape[0], block), lambda i: (0, i)) for p in [*mine, *other]]
    column = lambda rows: pl.BlockSpec((rows, block), lambda i: (0, i))
    square = pl.BlockSpec((1, block, block), lambda i: (i, 0, 0))
    return pl.pallas_call(
        functools.partial(recurrence_kernel, len(mine)),
        grid=(blocks,),
        in_specs=[
            pl.BlockSpec(memory_space=pltpu.SMEM),
            pl.BlockSpec((length, width), lambda i: (0, 0)),
            column(taps.shape[0]),
            square,
            square,
            column(1),
            column(length),
            *parts,
        ],
        out_specs=column(length),
        out_shape=jax.ShapeDtypeStruct((length, block * blocks), jnp.bfloat16),
        cost_estimate=pl.CostEstimate(
            flops=4 * length * width * block * blocks,
            bytes_accessed=4 * width * block * blocks + 8 * length * block * blocks,
            transcendentals=0,
        ),
        compiler_params=pltpu.CompilerParams(vmem_limit_bytes=VMEM_BYTES),
    )(meta, tokens, taps, rate_blocks, inlet_blocks, plus, shift, *mine, *other)


def hidden_kernel(count, meta, x_ref, *refs):
    mine, other, out_ref = refs[:count], refs[count : 2 * count], refs[-1]
    first = split_product(meta, x_ref, mine)
    second = split_product(meta, x_ref, other)
    swapped = meta[0] == 1
    gate = jnp.where(swapped, second, first)
    upward = jnp.where(swapped, first, second)
    out_ref[...] = (gate * sigmoid(gate) * upward).astype(jnp.bfloat16)


def hidden_units(normed, mine, other, meta):
    length, width = normed.shape
    units = mine[0].shape[1]
    tile = next(t for t in (512, 640, 256, 128, units) if units % t == 0)
    return pl.pallas_call(
        functools.partial(hidden_kernel, len(mine)),
        grid=(units // tile,),
        in_specs=[
            pl.BlockSpec(memory_space=pltpu.SMEM),
            pl.BlockSpec((length, width), lambda i: (0, 0)),
            *[pl.BlockSpec((p.shape[0], tile), lambda i: (0, i)) for p in [*mine, *other]],
        ],
        out_specs=pl.BlockSpec((length, tile), lambda i: (0, i)),
        out_shape=jax.ShapeDtypeStruct((length, units), jnp.bfloat16),
        cost_estimate=pl.CostEstimate(
            flops=4 * length * width * units, bytes_accessed=4 * width * units, transcendentals=0
        ),
        compiler_params=pltpu.CompilerParams(vmem_limit_bytes=VMEM_BYTES),
    )(meta, normed, *mine, *other)


def outward_kernel(count, meta, left_ref, *refs):
    mine, other, out_ref = refs[:count], refs[count : 2 * count], refs[-1]
    half = mine[0].shape[0]
    near = pl.ds(pl.multiple_of(meta[0] * half, 128), half)
    far = pl.ds(pl.multiple_of((1 - meta[0]) * half, 128), half)
    start = 0
    for at in range(count):
        total = jnp.dot(left_ref[:, near], mine[at][...], preferred_element_type=jnp.float32)
        total += jnp.dot(left_ref[:, far], other[at][...], preferred_element_type=jnp.float32)
        columns = mine[at].shape[1]
        out_ref[:, start : start + columns] = total.astype(jnp.bfloat16)
        start += columns


def outward(left, mine, other, meta):
    length, depth = left.shape
    width = sum(p.shape[1] for p in mine)
    rows = min(length, 256)
    whole = [pl.BlockSpec(p.shape, lambda i: (0, 0)) for p in [*mine, *other]]
    return pl.pallas_call(
        functools.partial(outward_kernel, len(mine)),
        grid=(length // rows,),
        in_specs=[
            pl.BlockSpec(memory_space=pltpu.SMEM),
            pl.BlockSpec((rows, depth), lambda i: (i, 0)),
            *whole,
        ],
        out_specs=pl.BlockSpec((rows, width), lambda i: (i, 0)),
        out_shape=jax.ShapeDtypeStruct((length, width), jnp.bfloat16),
        cost_estimate=pl.CostEstimate(
            flops=2 * length * width * depth, bytes_accessed=2 * width * depth, transcendentals=0
        ),
        compiler_params=pltpu.CompilerParams(vmem_limit_bytes=VMEM_BYTES),
    )(meta, left, *mine, *other)


def add_groups(terms):
    groups = lax.axis_size("tp")
    if groups != 2:
        return lax.psum_scatter(terms, "tp", scatter_dimension=0, tiled=True).astype(jnp.float32)
    share = terms.shape[0] // 2
    me = lax.axis_index("tp")
    away = lax.dynamic_slice_in_dim(terms, (1 - me) * share, share, 0)
    own = lax.dynamic_slice_in_dim(terms, me * share, share, 0)
    came = lax.ppermute(away, "tp", [(0, 1), (1, 0)])
    return own.astype(jnp.float32) + came.astype(jnp.float32)


def grouped_outward(left, mine, other, owners, meta, cut):
    count = len(mine)
    if count == 1:
        return add_groups(outward(left, mine, other, meta))
    outer = count // 2
    chunks = [list(range(count))]
    if cut:
        steps = visit_order(outer)
        last, late = steps[-1], [outer + step for step in steps]
        early = [at for at in range(outer + 1) if at != last]
        chunks = [chunk for chunk in (early, late[:-1], [last], late[-1:]) if chunk]
    width = mine[0].shape[1]
    total = jnp.zeros((left.shape[0] // lax.axis_size("tp"), width * count), jnp.float32)
    for chunk in chunks:
        terms = outward(left, [mine[at] for at in chunk], [other[at] for at in chunk], meta)
        block = add_groups(terms)
        for place, at in enumerate(chunk):
            piece = block[:, place * width : (place + 1) * width]
            total = lax.dynamic_update_slice_in_dim(total, piece, owners[at] * width, 1)
    return total


def all_rows(rows):
    if lax.axis_size("tp") != 2:
        return lax.all_gather(rows, "tp", axis=0, tiled=True)
    came = lax.ppermute(rows, "tp", [(0, 1), (1, 0)])
    low = lax.axis_index("tp") == 0
    return jnp.concatenate([jnp.where(low, rows, came), jnp.where(low, came, rows)], axis=0)


def layer(
    tokens,
    recurrence_branch_weight,
    gate_branch_weight,
    convolution_kernel,
    recurrence_gate_blockwise,
    input_gate_blockwise,
    channel_decay_param,
    token_decay_shift,
    recurrence_output_weight,
    first_norm_gain,
    feedforward_gate_weight,
    feedforward_up_weight,
    feedforward_down_weight,
    second_norm_gain,
):
    share = tokens.shape[0] // lax.axis_size("tp")
    offset = lax.axis_index("tp") * share
    in_mine, in_other, owners, swapped = gather_two(recurrence_branch_weight, gate_branch_weight, 0)
    out_mine, out_other, _, _ = gather_halves(recurrence_output_weight)
    ff_mine, ff_other, _, _ = gather_two(feedforward_gate_weight, feedforward_up_weight, 0)
    down_mine, down_other, _, _ = gather_halves(feedforward_down_weight)
    meta = scalars(owners, swapped)
    branch = recurrence(
        tokens,
        in_mine,
        in_other,
        meta,
        convolution_kernel,
        recurrence_gate_blockwise,
        input_gate_blockwise,
        jax.nn.softplus(-channel_decay_param)[None, :],
        token_decay_shift,
    )
    mix = grouped_outward(branch, out_mine, out_other, owners, meta, False)
    own_tokens = lax.dynamic_slice_in_dim(tokens, offset, share, 0)
    normed = layer_norm(
        residual_scale * own_tokens.astype(jnp.float32) + mix, first_norm_gain
    ).astype(jnp.bfloat16)
    rows = all_rows(normed)
    hidden = hidden_units(rows, ff_mine, ff_other, meta)
    ffn = grouped_outward(hidden, down_mine, down_other, owners, meta, True)
    return layer_norm(residual_scale * normed.astype(jnp.float32) + ffn, second_norm_gain).astype(
        jnp.bfloat16
    )


def solution(mesh):
    return jax.shard_map(
        layer,
        mesh=mesh,
        in_specs=(
            P(("rep", "fs"), None),
            P("fs", "tp"),
            P("fs", "tp"),
            P(None, "tp"),
            P("tp", None, None),
            P("tp", None, None),
            P("tp"),
            P(("rep", "fs"), "tp"),
            P("tp", "fs"),
            P(),
            P("fs", "tp"),
            P("fs", "tp"),
            P("tp", "fs"),
            P(),
        ),
        out_specs=P(("rep", "fs", "tp"), None),
        check_vma=False,
    )
```
